32 devices in a mesh: sp: 16 (over z, y, x), tp: 2 (over core).
Axes of the slice: x: 2, y: 2, z: 4, core: 2. Of those that a mesh axis runs over, the one named last changes fastest.
Arguments:
- moe_input: bfloat16 [4096, 2048], P('sp'), may hold values from -6 to 6
- cotangent: bfloat16 [4096, 2048], P('sp'), may hold values from -6 to 6
- expert_ids: int32 [4096, 2], P('sp'), may hold values from 0 to 15, all different within a row; in each aligned block of 256 rows (0 to 255, 256 to 511, ...) at most 64 rows name the same one
- route_weight: float32 [4096, 2], P('sp'), may hold values from 0.05 to 0.6
- gate_proj: bfloat16 [16, 2048, 1024], P('sp', None, 'tp'), may hold values from -0.125 to 0.125
- up_proj: bfloat16 [16, 2048, 1024], P('sp', None, 'tp'), may hold values from -0.125 to 0.125
- down_proj: bfloat16 [16, 1024, 2048], P('sp', 'tp'), may hold values from -0.1875 to 0.1875
- out_weight: bfloat16 [2048, 2048], P(None, 'tp'), may hold values from -0.125 to 0.125
- recur_input: bfloat16 [4096, 2048], P('sp', 'tp'), may hold values from -6 to 6
- gate_input: bfloat16 [4096, 2048], P('sp', 'tp'), may hold values from -6 to 6
- states: float32 [4096, 2048], P('sp', 'tp'), may hold values from -6 to 6
- conv_taps: bfloat16 [4, 2048], P(None, 'tp'), may hold values from -3 to 3
- decay_gate_w: bfloat16 [16, 128, 128], P('tp'), may hold values from -0.5 to 0.5
- input_gate_w: bfloat16 [16, 128, 128], P('tp'), may hold values from -0.5 to 0.5
- decay_rate: float32 [2048], P('tp'), may hold values from 7.3242187e-06 to 0.008
- decay_extra: float32 [4096, 2048], P('sp', 'tp'), may hold values from -0.77 to 0
Outputs:
- gate_proj_grad: bfloat16 [16, 2048, 1024], P('sp', None, 'tp')
- up_proj_grad: bfloat16 [16, 2048, 1024], P('sp', None, 'tp')
- down_proj_grad: bfloat16 [16, 1024, 2048], P('sp', 'tp')
- out_weight_grad: float32 [2048, 2048], P('sp', 'tp')
- input_grad: bfloat16 [4096, 2048], P('sp')
- recur_grad: bfloat16 [4096, 2048], P('sp', 'tp')
- gate_grad: bfloat16 [4096, 2048], P('sp', 'tp')
The draws below stay inside these ranges and needn't reach their ends.
Inputs may be any that keep to these rules, and one draw needn't show every extreme that they name: `expert_ids`: within each aligned block of 256 tokens a token names 2 different experts, and no expert is named more than 64 times.
All inputs are finite; a program needn't handle non-finite values.
Results may differ from the reference program's by a relative error of at most 0.012.
Values may be sent and summed in bfloat16 or wider, within the bound.
A program may use at most 128 MiB of HBM per device.

```python
import math
import jax
import jax.numpy as jnp
import numpy as np
from jax import lax

D = 2048
FF = 1024
RECURRENCE_WIDTH = 2048
LRU_BLOCKS = 16
TOPK = 2
TOK_DEV = 256
BLK = 128
SEQUENCE_TOKENS = 4096
EXPERTS = 16
CAP = 64
N_SP = 16
N_TP = 2


def decay_parts(key):
    base_key = jax.random.fold_in(key, 4242)
    multiple_count = jax.random.split(base_key, 6)
    fast_share = 0.5
    fast_mask = jax.random.uniform(multiple_count[0], (RECURRENCE_WIDTH,), jnp.float32) < fast_share
    slow_rate = jnp.exp(jax.random.uniform(multiple_count[1], (RECURRENCE_WIDTH,), jnp.float32, math.log(0.03 / SEQUENCE_TOKENS), math.log(0.15 / SEQUENCE_TOKENS)))
    fast_rate = jnp.exp(jax.random.uniform(multiple_count[2], (RECURRENCE_WIDTH,), jnp.float32, math.log(0.0025), math.log(0.008)))
    rate_value = jnp.where(fast_mask, fast_rate, slow_rate)
    block_count = SEQUENCE_TOKENS // TOK_DEV
    factor = jax.random.uniform(multiple_count[3], (block_count, RECURRENCE_WIDTH), jnp.float32, 0.0, 2.0)
    gentle_component = jnp.repeat(-4.0 * rate_value[None, :] * factor, TOK_DEV, axis=0)
    spike_indicator = jax.random.uniform(multiple_count[4], (SEQUENCE_TOKENS, RECURRENCE_WIDTH), jnp.float32) < 3.0 / SEQUENCE_TOKENS
    spike_magnitude = jax.random.uniform(multiple_count[5], (SEQUENCE_TOKENS, RECURRENCE_WIDTH), jnp.float32, 0.22, 0.7)
    additional_value = gentle_component - jnp.where(spike_indicator, spike_magnitude, 0.0)
    return (rate_value, additional_value)


def draw_decay_rate(key, part):
    return decay_parts(key)[0]


def draw_decay_extra(key, part):
    return decay_parts(key)[1]


def with_spikes(drawn, own_key, source, target, blocks, factor):
    def block_of(axis_at):
        return (jnp.arange(drawn.shape[axis_at]) // (drawn.shape[axis_at] // blocks)).reshape((-1,) + (1,) * (drawn.ndim - 1 - axis_at))

    near = jax.random.permutation(own_key, blocks)[block_of(target)]
    second = (block_of(target) + blocks // 2) % blocks
    return jnp.where((block_of(source) == near) | (block_of(source) == second), factor * drawn, drawn)


def levels(key, shape, shards, low, high):
    def one(axis_at, shards_of):
        draws = jax.random.uniform(jax.random.fold_in(jax.random.fold_in(key, 6), axis_at), (shards_of,), jnp.float32, low / len(shards), high / len(shards))
        return jnp.repeat(jnp.exp(draws), shape[axis_at] // shards_of).reshape((-1,) + (1,) * (len(shape) - axis_at - 1))

    loudness = one(*shards[0])
    for cut in shards[1:]:
        loudness = loudness * one(*cut)
    return loudness


def shared_out(own_key, own, number, rows, count, top, limit, lean):
    order = jax.random.permutation(own_key, count)
    heavy_load, ordinary = shares(count, rows * top, limit, lean, True), shares(count, rows * top, limit, lean, False)
    places = jnp.arange(count)

    def named(sizes, turn):
        used = int((sizes > 0).sum())
        fixed = max(1, used // 4)
        passed = fixed + (places - fixed + turn * (used - fixed)) % max(1, count - fixed)
        return jnp.zeros((count,), jnp.int32).at[order[jnp.where(places < fixed, places, passed)]].set(jnp.asarray(sizes, jnp.int32))

    sizes = jnp.where(number % 4 == 0, named(heavy_load, number // 4), named(ordinary, number - number // 4 - 1))
    mixed = jax.random.permutation(jax.random.fold_in(own, 3), count)
    donor, taker = mixed[0:count // 2 * 2:2], mixed[1:count // 2 * 2:2]
    margin = jnp.minimum(sizes[donor] - 1, limit - sizes[taker]) // 2
    margin = jnp.where((donor == order[0]) | (taker == order[0]) | (sizes[taker] == 0), 0, jnp.maximum(margin, 0))
    passed = jax.random.randint(jax.random.fold_in(own, 4), (count // 2,), 0, 1 << 20) % (margin + 1)
    sizes = sizes.at[donor].add(-passed).at[taker].add(passed)
    items = jnp.searchsorted(jnp.cumsum(sizes), jnp.arange(rows * top), side="right").astype(jnp.int32)
    grid = items.reshape(top, rows).T
    grid = grid[jax.random.permutation(jax.random.fold_in(own, 1), rows)]
    turn = jax.random.randint(jax.random.fold_in(own, 2), (rows, 1), 0, top)
    return jnp.take_along_axis(grid, (jnp.arange(top)[None, :] + turn) % top, axis=1)


def shares(amount, total, limit, lean, full):
    loads = [(1 << 20) // math.isqrt(rank ** lean) + 1 for rank in range(1, amount + 1)]
    largest = limit if full else min(limit, max(-(-total // amount), total * loads[0] // sum(loads)))
    least = 1 if total - largest >= amount - 1 else 0
    holding, surplus = [largest] + [least] * (amount - 1), total - largest - least * (amount - 1)
    while surplus > 0:
        free = [i for i in range(1, amount) if holding[i] < largest] or [i for i in range(1, amount) if holding[i] < limit]
        whole, left = sum([loads[i] for i in free]), surplus
        for i in free:
            extra = min(limit - holding[i], max(1, left * loads[i] // whole), surplus)
            holding[i] = holding[i] + extra
            surplus = surplus - extra
    return np.array(holding)


def bell_draw(key, dims, width, reach, cuts=(), kind=jnp.bfloat16):
    entries = width * jax.random.normal(key, dims, jnp.float32)
    if cuts:
        entries = entries * levels(key, dims, cuts, -0.22, 0.18)
    return jnp.clip(entries, -reach, reach).astype(kind)


def heavy_noise(own_key, shape, deviation, most, pieces, heavy, kind=jnp.bfloat16):
    values = deviation * jax.random.normal(own_key, shape, jnp.float32)
    if pieces:
        values = values * levels(own_key, shape, pieces, -0.22, 0.18)
    return jnp.clip(with_spikes(values, jax.random.fold_in(own_key, 3), *heavy), -most, most).astype(kind)


def setup_inputs(seed: int = 0) -> dict:
    keys = jax.random.split(jax.random.key(seed), 17)
    moe_input = bell_draw(keys[0], (SEQUENCE_TOKENS, D), 1.0, 6.0, ((0, 16),))
    cotangent = heavy_noise(keys[1], (SEQUENCE_TOKENS, D), 1.0, 6.0, ((0, 16),), (0, 1, 16, 2.0))
    expert_ids_keys = jax.random.split(jax.random.fold_in(keys[2], 1), SEQUENCE_TOKENS // TOK_DEV)
    expert_ids_turns = jax.random.permutation(jax.random.fold_in(keys[2], 3), SEQUENCE_TOKENS // TOK_DEV)
    expert_ids = jax.vmap(lambda own, number: shared_out(jax.random.fold_in(keys[2], 2), own, number, TOK_DEV, EXPERTS, TOPK, CAP, 1))(expert_ids_keys, expert_ids_turns).reshape((SEQUENCE_TOKENS, TOPK))
    route_weight = jnp.clip(0.05 + 0.55 * jax.random.uniform(keys[3], (SEQUENCE_TOKENS, TOPK), jnp.float32) ** levels(keys[3], (SEQUENCE_TOKENS, TOPK), ((0, 16),), -0.2, 0.2), 0.05, 0.6)
    gate_proj = bell_draw(keys[4], (EXPERTS, D, FF), D ** -0.5, 0.125, ((0, 16), (2, 2)))
    up_proj = bell_draw(keys[5], (EXPERTS, D, FF), D ** -0.5, 0.125, ((0, 16), (2, 2)))
    down_proj = bell_draw(keys[6], (EXPERTS, FF, D), FF ** -0.5, 0.1875, ((0, 16), (1, 2)))
    out_weight = bell_draw(keys[7], (D, RECURRENCE_WIDTH), RECURRENCE_WIDTH ** -0.5, 0.125, ((1, 2),))
    recur_input = bell_draw(keys[8], (SEQUENCE_TOKENS, RECURRENCE_WIDTH), 1.0, 6.0, ((0, 16), (1, 2)))
    gate_input = bell_draw(keys[9], (SEQUENCE_TOKENS, RECURRENCE_WIDTH), 1.0, 6.0, ((0, 16), (1, 2)))
    states = bell_draw(keys[10], (SEQUENCE_TOKENS, RECURRENCE_WIDTH), 1.0, 6.0, ((0, 16), (1, 2)), jnp.float32)
    conv_taps = bell_draw(keys[11], (4, RECURRENCE_WIDTH), 4 ** -0.5, 3.0, ((1, 2),))
    decay_gate_w = bell_draw(keys[12], (LRU_BLOCKS, BLK, BLK), BLK ** -0.5, 0.5, ((0, 2),))
    input_gate_w = bell_draw(keys[13], (LRU_BLOCKS, BLK, BLK), BLK ** -0.5, 0.5, ((0, 2),))
    decay_rate = draw_decay_rate(jax.random.fold_in(keys[16], 71), 0)
    decay_extra = draw_decay_extra(jax.random.fold_in(keys[16], 71), 0)
    return dict(moe_input=moe_input, cotangent=cotangent, expert_ids=expert_ids, route_weight=route_weight, gate_proj=gate_proj, up_proj=up_proj, down_proj=down_proj, out_weight=out_weight, recur_input=recur_input, gate_input=gate_input, states=states, conv_taps=conv_taps, decay_gate_w=decay_gate_w, input_gate_w=input_gate_w, decay_rate=decay_rate, decay_extra=decay_extra)


decay_scale = 8.0

def pair_combine(earlier, later):
    return (earlier[0] * later[0], later[0] * earlier[1] + later[1])

def rounded(value):
    return lax.optimization_barrier(value.astype(jnp.bfloat16)).astype(jnp.float32)

def slot_layout(expert_ids):
    source_ids = expert_ids.reshape(N_SP, TOK_DEV * TOPK)
    onehot = (source_ids[:, :, None] == jnp.arange(EXPERTS, dtype=jnp.int32)[None, None, :]).astype(jnp.int32)
    slot_rank = lax.optimization_barrier(jnp.sum((jnp.cumsum(onehot, axis=1) - onehot) * onehot, axis=2))
    sources = jnp.arange(N_SP, dtype=jnp.int32)[:, None]
    target = ((source_ids * N_SP + sources) * CAP + slot_rank).reshape(-1).astype(jnp.int32)
    source_table = jnp.full((EXPERTS * N_SP * CAP,), SEQUENCE_TOKENS * TOPK, jnp.int32)
    source_table = source_table.at[target].set(jnp.arange(SEQUENCE_TOKENS * TOPK, dtype=jnp.int32))
    return (source_table.reshape(EXPERTS, N_SP * CAP), target)

def reference(moe_input, cotangent, expert_ids, route_weight, gate_proj, up_proj, down_proj, out_weight, recur_input, gate_input, states, conv_taps, decay_gate_w, input_gate_w, decay_rate, decay_extra):
    cot_float = cotangent.astype(jnp.float32)
    scaled = (route_weight[:, :, None] * cot_float[:, None, :]).astype(jnp.bfloat16).reshape(SEQUENCE_TOKENS * TOPK, D)
    token_rows = jnp.repeat(moe_input, TOPK, axis=0)
    zero_row = jnp.zeros((1, D), jnp.bfloat16)
    padded_rows = jnp.concatenate([token_rows, zero_row], axis=0)
    padded_cot = jnp.concatenate([scaled, zero_row], axis=0)
    source_table, target = slot_layout(expert_ids)

    def one_expert(inputs):
        slot_index, weight_gate, weight_up, weight_down = inputs
        rows_float = padded_rows[slot_index].astype(jnp.float32)
        cot_rows = padded_cot[slot_index].astype(jnp.float32)
        gate_float = weight_gate.astype(jnp.float32)
        up_float = weight_up.astype(jnp.float32)
        down_float = weight_down.astype(jnp.float32)
        gate_pre = jnp.dot(rows_float, gate_float)
        up_pre = jnp.dot(rows_float, up_float)
        sigmoid_gate = jax.nn.sigmoid(gate_pre)
        silu_gate = gate_pre * sigmoid_gate
        hidden = rounded(silu_gate * up_pre)
        down_grad = jnp.dot(hidden.T, cot_rows)
        hidden_grad = jnp.dot(cot_rows, down_float.T)
        gate_pre_grad = rounded(hidden_grad * up_pre * sigmoid_gate * (1.0 + gate_pre * (1.0 - sigmoid_gate)))
        up_pre_grad = rounded(hidden_grad * silu_gate)
        gate_weight_grad = jnp.dot(rows_float.T, gate_pre_grad)
        up_weight_grad = jnp.dot(rows_float.T, up_pre_grad)
        share_size = FF // N_TP
        summed = jnp.zeros((N_SP * CAP, D), jnp.float32)
        for part_index in range(N_TP):
            lower = part_index * share_size
            upper = lower + share_size
            piece_grad = jnp.dot(gate_pre_grad[:, lower:upper], gate_float[:, lower:upper].T) + jnp.dot(up_pre_grad[:, lower:upper], up_float[:, lower:upper].T)
            summed = summed + rounded(piece_grad)
        return (gate_weight_grad.astype(jnp.bfloat16), up_weight_grad.astype(jnp.bfloat16), down_grad.astype(jnp.bfloat16), summed.astype(jnp.bfloat16))
    gate_proj_grad, up_proj_grad, down_proj_grad, slot_grad = lax.map(one_expert, (source_table, gate_proj, up_proj, down_proj))
    gathered = slot_grad.reshape(EXPERTS * N_SP * CAP, D)[target].astype(jnp.float32)
    gathered = gathered.reshape(SEQUENCE_TOKENS, TOPK, D)
    moe_grad = gathered[:, 0]
    for choice_index in range(1, TOPK):
        moe_grad = moe_grad + gathered[:, choice_index]
    input_grad = (moe_grad + cot_float).astype(jnp.bfloat16)
    grad_float = input_grad.astype(jnp.float32)
    gate_float_in = gate_input.astype(jnp.float32)
    gelu_value, gelu_back = jax.vjp(jax.nn.gelu, gate_float_in)
    mixer_out = (states * gelu_value).astype(jnp.bfloat16).astype(jnp.float32)
    out_weight_grad = jnp.dot(grad_float.T, mixer_out)
    mixer_grad = jnp.dot(grad_float, out_weight.astype(jnp.float32))
    gate_grad = gelu_back(mixer_grad * states)[0].astype(jnp.bfloat16)
    state_grad = mixer_grad * gelu_value
    taps = conv_taps.astype(jnp.float32)
    padded_in = jnp.pad(recur_input.astype(jnp.float32), ((3, 0), (0, 0)))
    conv = taps[0] * padded_in[0:SEQUENCE_TOKENS]
    for tap_index in range(1, 4):
        conv = conv + taps[tap_index] * padded_in[tap_index:tap_index + SEQUENCE_TOKENS]
    conv_blocks = rounded(conv).reshape(SEQUENCE_TOKENS, LRU_BLOCKS, BLK)
    decay_w = decay_gate_w.astype(jnp.float32)
    input_w = input_gate_w.astype(jnp.float32)
    decay_pre = jnp.einsum('tbi,bij->tbj', conv_blocks, decay_w).reshape(SEQUENCE_TOKENS, RECURRENCE_WIDTH)
    input_pre = jnp.einsum('tbi,bij->tbj', conv_blocks, input_w).reshape(SEQUENCE_TOKENS, RECURRENCE_WIDTH)
    recur_gate = jax.nn.sigmoid(decay_pre)
    input_gate = jax.nn.sigmoid(input_pre)
    positions = jnp.arange(SEQUENCE_TOKENS, dtype=jnp.int32)
    first_row = (positions == 0)[:, None]
    log_decay = -decay_scale * recur_gate * decay_rate[None, :] + decay_extra
    decay_value = jnp.exp(log_decay)
    mult = jnp.where(first_row, 1.0, jnp.sqrt(-jnp.expm1(2.0 * log_decay)))
    prev_states = jnp.concatenate([jnp.zeros((1, RECURRENCE_WIDTH), jnp.float32), states[:-1]], axis=0)
    next_decay = jnp.concatenate([decay_value[1:], jnp.zeros((1, RECURRENCE_WIDTH), jnp.float32)], axis=0)
    cumul_flip, values_flip = lax.associative_scan(pair_combine, (next_decay[::-1], state_grad[::-1]), axis=0)
    carried_grad = values_flip[::-1]
    log_grad = carried_grad * prev_states * decay_value - jnp.where(first_row, 0.0, carried_grad * input_gate * conv * decay_value * decay_value / mult)
    decay_pre_grad = rounded(log_grad * (-decay_scale * decay_rate[None, :]) * recur_gate * (1.0 - recur_gate))
    input_pre_grad = rounded(carried_grad * mult * conv * input_gate * (1.0 - input_gate))
    conv_grad = carried_grad * mult * input_gate + jnp.einsum('tbj,bij->tbi', decay_pre_grad.reshape(SEQUENCE_TOKENS, LRU_BLOCKS, BLK), decay_w).reshape(SEQUENCE_TOKENS, RECURRENCE_WIDTH) + jnp.einsum('tbj,bij->tbi', input_pre_grad.reshape(SEQUENCE_TOKENS, LRU_BLOCKS, BLK), input_w).reshape(SEQUENCE_TOKENS, RECURRENCE_WIDTH)
    padded_grad = jnp.pad(conv_grad, ((0, 3), (0, 0)))
    recur_float = taps[0] * padded_grad[3:3 + SEQUENCE_TOKENS]
    for tap_index in range(1, 4):
        recur_float = recur_float + taps[tap_index] * padded_grad[3 - tap_index:3 - tap_index + SEQUENCE_TOKENS]
    recur_grad = recur_float.astype(jnp.bfloat16)
    return (gate_proj_grad, up_proj_grad, down_proj_grad, out_weight_grad, input_grad, recur_grad, gate_grad)
```

```python
import jax
import jax.numpy as jnp
from jax import lax
from jax.experimental import pallas as pl
from jax.experimental.pallas import tpu as pltpu
from jax.sharding import PartitionSpec as P

decay_scale = 8.0


def passed_along(value, axis, steps):
    count = lax.axis_size(axis)
    initial, last = (max(0, -steps), min(count, count - steps))
    return lax.ppermute(value, axis, [(source, source + steps) for source in range(initial, last)])


def swapped(value, axis):
    return lax.ppermute(value, axis, [(0, 1), (1, 0)])


def carried_in(product, total, axis):
    count, mine = (lax.axis_size(axis), lax.axis_index(axis))
    pair = jnp.stack([product, total])
    pieces = lax.all_to_all(
        jnp.broadcast_to(pair[None], (count,) + pair.shape),
        axis,
        split_axis=0,
        concat_axis=0,
        tiled=True,
    )
    entering = jnp.zeros_like(total)
    for position in range(count - 1, 0, -1):
        longer = pieces[position, 0] * entering + pieces[position, 1]
        entering = jnp.where(position > mine, longer, entering)
    return entering


def scan_kernel(decay_ref, grad_ref, product_ref, local_ref):
    rows, lanes = decay_ref.shape
    group = 8
    last = rows // group - 1

    def step(index, carry):
        product, total, decay = carry
        start = pl.multiple_of((last - index) * group, group)
        decays = decay_ref[pl.ds(start, group), :]
        grads = grad_ref[pl.ds(start, group), :]
        products, totals = ([None] * group, [None] * group)
        for row in range(group - 1, -1, -1):
            product = product * decay
            total = grads[row : row + 1] + decay * total
            decay = decays[row : row + 1]
            products[row], totals[row] = (product, total)
        product_ref[pl.ds(start, group), :] = jnp.concatenate(products, axis=0)
        local_ref[pl.ds(start, group), :] = jnp.concatenate(totals, axis=0)
        return (product, total, decay)

    one = jnp.ones((1, lanes), jnp.float32)
    lax.fori_loop(0, last + 1, step, (one, jnp.zeros_like(one), one))


def reverse_scan(decay, grad):
    rows, channels = decay.shape
    width = 512 if channels % 512 == 0 else channels
    block = pl.BlockSpec((rows, width), lambda index: (0, index))
    return pl.pallas_call(
        scan_kernel,
        grid=(channels // width,),
        in_specs=[block, block],
        out_specs=[block, block],
        out_shape=[jax.ShapeDtypeStruct(decay.shape, jnp.float32)] * 2,
        cost_estimate=pl.CostEstimate(
            flops=3 * rows * channels, bytes_accessed=16 * rows * channels, transcendentals=0
        ),
        name="reverse_scan",
    )(decay, grad)


def contract_rows(left, right):
    return lax.dot_general(
        left, right, (((0,), (0,)), ((), ())), preferred_element_type=jnp.float32
    )


def contract_cols(left, right):
    return lax.dot_general(
        left, right, (((1,), (1,)), ((), ())), preferred_element_type=jnp.float32
    )


def on_device(
    moe_input,
    cotangent,
    expert_ids,
    route_weight,
    gate_proj,
    up_proj,
    down_proj,
    out_weight,
    recur_input,
    gate_input,
    states,
    conv_taps,
    decay_gate_w,
    input_gate_w,
    decay_rate,
    decay_extra,
):
    experts = lax.axis_size("sp")
    cores = lax.axis_size("tp")
    tok_rows, width = moe_input.shape
    top_count = expert_ids.shape[1]
    capacity = max(2, 4 * tok_rows // experts)
    slot_count = experts * capacity
    gate_float = gate_input.astype(jnp.float32)
    gelu_value, gelu_back = jax.vjp(jax.nn.gelu, gate_float)
    mixer_out = (states * gelu_value).astype(jnp.bfloat16)
    mixer_all = lax.all_gather(mixer_out, "sp", axis=0, tiled=True)
    flat_ids = expert_ids.reshape(-1)
    onehot = (flat_ids[:, None] == jnp.arange(experts, dtype=jnp.int32)[None, :]).astype(jnp.int32)
    slot_rank = jnp.sum((jnp.cumsum(onehot, axis=0) - onehot) * onehot, axis=1)
    target = flat_ids * capacity + slot_rank
    slot_iota = jnp.arange(slot_count, dtype=jnp.int32)
    placing = (slot_iota[:, None] == target[None, :]).astype(jnp.bfloat16)
    pair_slots = target.reshape(tok_rows, top_count)
    placing_tok = jnp.any(slot_iota[:, None, None] == pair_slots[None, :, :], axis=2).astype(
        jnp.bfloat16
    )
    scaled = (route_weight[:, :, None] * cotangent.astype(jnp.float32)[:, None, :]).astype(
        jnp.bfloat16
    )
    scaled = scaled.reshape(tok_rows * top_count, width)
    send_rows = jnp.dot(placing_tok, moe_input, preferred_element_type=jnp.float32).astype(
        jnp.bfloat16
    )
    send_rows = send_rows.reshape(experts, capacity, width)
    send_grads = jnp.dot(placing, scaled, preferred_element_type=jnp.float32).astype(jnp.bfloat16)
    send_grads = send_grads.reshape(experts, capacity, width)
    share_size = capacity // cores
    offset = lax.axis_index("tp") * share_size
    mine_rows = lax.dynamic_slice_in_dim(send_rows, offset, share_size, 1)
    mine_grads = lax.dynamic_slice_in_dim(send_grads, offset, share_size, 1)
    got_rows = lax.all_to_all(mine_rows, "sp", split_axis=0, concat_axis=0, tiled=True)
    got_grads = lax.all_to_all(mine_grads, "sp", split_axis=0, concat_axis=0, tiled=True)
    got_rows = got_rows.reshape(experts * share_size, width)
    got_grads = got_grads.reshape(experts * share_size, width)
    rows_in = jnp.concatenate([got_rows, swapped(got_rows, "tp")], axis=0)
    grads_in = jnp.concatenate([got_grads, swapped(got_grads, "tp")], axis=0)
    weight_gate = gate_proj[0]
    weight_up = up_proj[0]
    weight_down = down_proj[0]
    gate_pre = jnp.dot(rows_in, weight_gate, preferred_element_type=jnp.float32)
    up_pre = jnp.dot(rows_in, weight_up, preferred_element_type=jnp.float32)
    sigmoid_gate = jax.nn.sigmoid(gate_pre)
    silu_gate = gate_pre * sigmoid_gate
    hidden = (silu_gate * up_pre).astype(jnp.bfloat16)
    down_grad = contract_rows(hidden, grads_in)
    hidden_grad = contract_cols(grads_in, weight_down)
    gate_pre_grad = (
        hidden_grad * up_pre * sigmoid_gate * (1.0 + gate_pre * (1.0 - sigmoid_gate))
    ).astype(jnp.bfloat16)
    up_pre_grad = (hidden_grad * silu_gate).astype(jnp.bfloat16)
    gate_weight_grad = contract_rows(rows_in, gate_pre_grad)
    up_weight_grad = contract_rows(rows_in, up_pre_grad)
    half = experts * share_size
    other_part = (
        contract_cols(gate_pre_grad[half:], weight_gate)
        + contract_cols(up_pre_grad[half:], weight_up)
    ).astype(jnp.bfloat16)
    arrived_part = swapped(other_part, "tp").astype(jnp.float32)
    own_part = contract_cols(gate_pre_grad[:half], weight_gate) + contract_cols(
        up_pre_grad[:half], weight_up
    )
    shared = (own_part + arrived_part).astype(jnp.bfloat16)
    shared, mixer_all = lax.optimization_barrier((shared, mixer_all))
    back_half = lax.all_to_all(
        shared.reshape(experts, share_size, width), "sp", split_axis=0, concat_axis=0, tiled=True
    )
    placing_half = lax.dynamic_slice_in_dim(
        placing_tok.reshape(experts, capacity, tok_rows), offset, share_size, 1
    ).reshape(half, tok_rows)
    moe_part = contract_rows(placing_half, back_half.reshape(half, width)).astype(jnp.bfloat16)
    moe_grad = moe_part.astype(jnp.float32) + swapped(moe_part, "tp").astype(jnp.float32)
    input_grad = (moe_grad + cotangent.astype(jnp.float32)).astype(jnp.bfloat16)
    column_share = width // experts
    grad_columns = lax.all_to_all(
        input_grad.reshape(tok_rows, experts, column_share).transpose(1, 0, 2),
        "sp",
        split_axis=0,
        concat_axis=0,
        tiled=True,
    ).reshape(experts * tok_rows, column_share)
    out_weight_grad = contract_rows(grad_columns, mixer_all)
    mixer_grad = jnp.dot(input_grad, out_weight, preferred_element_type=jnp.float32)
    gate_grad = gelu_back(mixer_grad * states)[0].astype(jnp.bfloat16)
    state_grad = mixer_grad * gelu_value
    channels = recur_input.shape[1]
    prev_inputs, prev_state = passed_along(
        (recur_input[-3:].astype(jnp.float32), states[-1:]), "sp", 1
    )
    extended = jnp.concatenate([prev_inputs, recur_input.astype(jnp.float32)], axis=0)
    taps = conv_taps.astype(jnp.float32)
    conv = taps[0] * extended[0:tok_rows]
    for tap_index in range(1, 4):
        conv = conv + taps[tap_index] * extended[tap_index : tap_index + tok_rows]
    blocks = decay_gate_w.shape[0]
    block_width = decay_gate_w.shape[1]
    conv_blocks = conv.astype(jnp.bfloat16).reshape(tok_rows, blocks, block_width)
    decay_pre = jnp.einsum(
        "tbi,bij->tbj", conv_blocks, decay_gate_w, preferred_element_type=jnp.float32
    ).reshape(tok_rows, channels)
    input_pre = jnp.einsum(
        "tbi,bij->tbj", conv_blocks, input_gate_w, preferred_element_type=jnp.float32
    ).reshape(tok_rows, channels)
    recur_gate = jax.nn.sigmoid(decay_pre)
    input_gate = jax.nn.sigmoid(input_pre)
    positions = lax.axis_index("sp") * tok_rows + jnp.arange(tok_rows, dtype=jnp.int32)
    first_row = (positions == 0)[:, None]
    log_decay = -decay_scale * recur_gate * decay_rate[None, :] + decay_extra
    decay_value = jnp.exp(log_decay)
    mult = jnp.where(first_row, 1.0, jnp.sqrt(-jnp.expm1(2.0 * log_decay)))
    prev_states = jnp.concatenate([prev_state, states[:-1]], axis=0)
    cumul, local_values = reverse_scan(decay_value, state_grad)
    entering = carried_in(decay_value[0] * cumul[0], decay_value[0] * local_values[0], "sp")
    carried_grad = local_values + cumul * entering[None, :]
    log_grad = carried_grad * prev_states * decay_value - jnp.where(
        first_row, 0.0, carried_grad * input_gate * conv * decay_value * decay_value / mult
    )
    decay_pre_grad = (
        log_grad * (-decay_scale * decay_rate[None, :]) * recur_gate * (1.0 - recur_gate)
    ).astype(jnp.bfloat16)
    input_pre_grad = (carried_grad * mult * conv * input_gate * (1.0 - input_gate)).astype(
        jnp.bfloat16
    )
    conv_grad = (
        carried_grad * mult * input_gate
        + jnp.einsum(
            "tbj,bij->tbi",
            decay_pre_grad.reshape(tok_rows, blocks, block_width),
            decay_gate_w,
            preferred_element_type=jnp.float32,
        ).reshape(tok_rows, channels)
        + jnp.einsum(
            "tbj,bij->tbi",
            input_pre_grad.reshape(tok_rows, blocks, block_width),
            input_gate_w,
            preferred_element_type=jnp.float32,
        ).reshape(tok_rows, channels)
    )
    next_grads = passed_along(conv_grad[:3], "sp", -1)
    grad_extended = jnp.concatenate([conv_grad, next_grads], axis=0)
    recur_float = taps[0] * grad_extended[3 : 3 + tok_rows]
    for tap_index in range(1, 4):
        recur_float = (
            recur_float + taps[tap_index] * grad_extended[3 - tap_index : 3 - tap_index + tok_rows]
        )
    recur_grad = recur_float.astype(jnp.bfloat16)
    return (
        gate_weight_grad.astype(jnp.bfloat16)[None],
        up_weight_grad.astype(jnp.bfloat16)[None],
        down_grad.astype(jnp.bfloat16)[None],
        out_weight_grad,
        input_grad,
        recur_grad,
        gate_grad,
    )


def solution(mesh):
    return jax.shard_map(
        on_device,
        mesh=mesh,
        in_specs=(
            P("sp", None),
            P("sp", None),
            P("sp", None),
            P("sp", None),
            P("sp", None, "tp"),
            P("sp", None, "tp"),
            P("sp", "tp", None),
            P(None, "tp"),
            P("sp", "tp"),
            P("sp", "tp"),
            P("sp", "tp"),
            P(None, "tp"),
            P("tp", None, None),
            P("tp", None, None),
            P("tp"),
            P("sp", "tp"),
        ),
        out_specs=(
            P("sp", None, "tp"),
            P("sp", None, "tp"),
            P("sp", "tp", None),
            P("sp", "tp"),
            P("sp", None),
            P("sp", "tp"),
            P("sp", "tp"),
        ),
        check_vma=False,
    )
```
